32 devices in a mesh: ep: 8 (over z, x), tp: 4 (over y, core).
Axes of the slice: x: 2, y: 2, z: 4, core: 2. Of those that a mesh axis runs over, the one named last changes fastest.
Arguments:
- queries: bfloat16 [6144, 1024], P('ep', 'tp'), may hold values from -6.5 to 6.5
- keys: bfloat16 [6144, 1024], P('ep', 'tp'), may hold values from -6.5 to 6.5
- values: bfloat16 [6144, 1024], P('ep', 'tp'), may hold values from -6 to 6
- cum_gate: float32 [6144, 16], P('ep', 'tp'), may hold values from -770 to 0, as said below
- head_gain: float32 [1024], P('tp'), may hold values from 0.1 to 1.9
- moe_in: bfloat16 [1024, 2048], P('ep'), may hold values from -6 to 6
- ffn_gain: float32 [2048], replicated, may hold values from 0.1 to 1.9
- routes: int32 [1024, 4], P('ep'), may hold values from 0 to 31, all different within a row; in each aligned block of 128 rows (0 to 127, 128 to 255, ...) at most 24 rows name the same one
- route_weight: float32 [1024, 4], P('ep'), may hold values from 0.2 to 1.2
- expert_gate: bfloat16 [32, 1024, 2048], P('ep', 'tp'), may hold values from -0.125 to 0.125
- expert_up: bfloat16 [32, 1024, 2048], P('ep', 'tp'), may hold values from -0.125 to 0.125
- expert_down: bfloat16 [32, 1024, 2048], P('ep', 'tp'), may hold values from -0.25 to 0.25
- shared_gate: bfloat16 [512, 2048], P('tp'), may hold values from -0.125 to 0.125
- shared_up: bfloat16 [512, 2048], P('tp'), may hold values from -0.125 to 0.125
- shared_down: bfloat16 [512, 2048], P('tp'), may hold values from -0.375 to 0.375
Outputs:
- mixed: bfloat16 [6144, 1024], P('ep', 'tp')
- expert_out: bfloat16 [1024, 2048], P('ep', 'tp')
The draws below stay inside these ranges and needn't reach their ends.
Inputs may be any that keep to these rules, and one draw needn't show every extreme that they name: `routes`: in each aligned block of 128 rows (the tokens of one index of ep) no expert is named by more than 24 rows, a bound that some block reaches; a row names 4 different experts. Each head's cum_gate never rises from one position to the next.
All inputs are finite; a program needn't handle non-finite values.
Results may differ from the reference program's by a relative error of at most 0.019.
Values may be sent and summed in bfloat16 or wider, within the bound.
A program may use at most 128 MiB of HBM per device.

```python
import math
import jax
import jax.numpy as jnp
import numpy as np
from jax import lax

D = 2048
HEADS = 16
HEAD = 64
FF_E = 1024
SHARED = 512
TOP = 4
ROWS = 768
MROWS = 128
SEQ = 6144
QW = 1024
MTOK = 1024
EXPERTS = 32
CAP = 24
N_EP = 8
N_TP = 4


def plant_pairs(key):
    base = jax.random.fold_in(key, 7)
    streams = jax.random.split(base, 2)
    query_rows = jnp.clip(jax.random.normal(streams[0], (SEQ, QW), jnp.float32), -6.0, 6.0)
    key_rows = jnp.clip(jax.random.normal(streams[1], (SEQ, QW), jnp.float32), -6.0, 6.0)
    return (query_rows, key_rows)


def draw_queries(key, part):
    return plant_pairs(key)[0].astype(jnp.bfloat16)


def draw_keys(key, part):
    return plant_pairs(key)[1].astype(jnp.bfloat16)


def draw_cum_gate(key, part):
    base = jax.random.fold_in(key, 11)
    streams = jax.random.split(base, 6)
    order = jax.random.permutation(streams[0], HEADS)
    slow_heads = order >= HEADS // 2
    fast_rate = jnp.exp(jax.random.uniform(streams[1], (HEADS,), jnp.float32, math.log(1.0 / 100.0), math.log(1.0 / 30.0)))
    fading_speed = jnp.where(slow_heads, 0.6 / SEQ, fast_rate)
    extent_coefficient = jnp.exp(jax.random.uniform(streams[2], (SEQ // ROWS,), jnp.float32, math.log(0.5), math.log(2.0)))
    extent_coefficient = jnp.repeat(extent_coefficient, ROWS)
    approximate_guess = jax.random.uniform(streams[3], (SEQ, HEADS), jnp.float32, 0.3, 1.7)
    spots = jax.random.randint(streams[4], (3,), 0, SEQ)
    discarded_items = jax.random.uniform(streams[5], (3, HEADS), jnp.float32, 0.22, 0.5)
    agreement_tally = (jnp.arange(SEQ)[:, None] == spots[None, :]).astype(jnp.float32)
    spike_occurrences = jnp.dot(agreement_tally, discarded_items)
    objective_list = fading_speed[None, :] * approximate_guess * extent_coefficient[:, None] + spike_occurrences
    return -jnp.cumsum(objective_list, axis=0)


def spiked(drawn, stream_key, source, target, parts, factor):
    def block_of(position):
        return (jnp.arange(drawn.shape[position]) // (drawn.shape[position] // parts)).reshape((-1,) + (1,) * (drawn.ndim - 1 - position))

    first = jax.random.permutation(stream_key, parts)[block_of(target)]
    second = (block_of(target) + parts // 2) % parts
    return jnp.where((block_of(source) == first) | (block_of(source) == second), factor * drawn, drawn)


def levels(stream_key, extent, cuts, smallest, top_value):
    level, own = 1.0, jax.random.fold_in(stream_key, 6)
    for axis_at, shards_of in cuts:
        draws = jnp.exp(jax.random.uniform(jax.random.fold_in(own, axis_at), (shards_of,), jnp.float32, smallest / len(cuts), top_value / len(cuts)))
        level = level * jnp.repeat(draws, extent[axis_at] // shards_of).reshape([-1 if axis == axis_at else 1 for axis in range(len(extent))])
    return level


def assign_block(own_key, own, number, rows, number_of, top, bound, skew):
    sequence = jax.random.permutation(own_key, number_of)
    heavy_load, common = load_shares(number_of, rows * top, bound, skew, True), load_shares(number_of, rows * top, bound, skew, False)
    places = jnp.arange(number_of)

    def named(tallies, offset_by):
        used = int((tallies > 0).sum())
        fixed = max(1, used // 4)
        passed = fixed + (places - fixed + offset_by * (used - fixed)) % max(1, number_of - fixed)
        return jnp.zeros((number_of,), jnp.int32).at[sequence[jnp.where(places < fixed, places, passed)]].set(jnp.asarray(tallies, jnp.int32))

    tallies = jnp.where(number % 4 == 0, named(heavy_load, number // 4), named(common, number - number // 4 - 1))
    mixed = jax.random.permutation(jax.random.fold_in(own, 3), number_of)
    giver, sink = mixed[0:number_of // 2 * 2:2], mixed[1:number_of // 2 * 2:2]
    slack = jnp.minimum(tallies[giver] - 1, bound - tallies[sink]) // 2
    slack = jnp.where((giver == sequence[0]) | (sink == sequence[0]) | (tallies[sink] == 0), 0, jnp.maximum(slack, 0))
    passed = jax.random.randint(jax.random.fold_in(own, 4), (number_of // 2,), 0, 1 << 20) % (slack + 1)
    tallies = tallies.at[giver].add(-passed).at[sink].add(passed)
    labels = jnp.searchsorted(jnp.cumsum(tallies), jnp.arange(rows * top), side="right").astype(jnp.int32)
    listing = labels.reshape(top, rows).T
    listing = listing[jax.random.permutation(jax.random.fold_in(own, 1), rows)]
    offset_by = jax.random.randint(jax.random.fold_in(own, 2), (rows, 1), 0, top)
    return jnp.take_along_axis(listing, (jnp.arange(top)[None, :] + offset_by) % top, axis=1)


def load_shares(amount, total, most, skew, full):
    portions = [(1 << 20) // math.isqrt(grade ** skew) + 1 for grade in range(1, amount + 1)]
    largest = most if full else min(most, max(-(-total // amount), total * portions[0] // sum(portions)))
    least = 1 if total - largest >= amount - 1 else 0
    counts, spare = [largest] + [least] * (amount - 1), total - largest - least * (amount - 1)
    while spare > 0:
        movable = [i for i in range(1, amount) if counts[i] < largest] or [i for i in range(1, amount) if counts[i] < most]
        whole, left = sum([portions[i] for i in movable]), spare
        for i in movable:
            more = min(most - counts[i], max(1, left * portions[i] // whole), spare)
            counts[i] = counts[i] + more
            spare = spare - more
    return np.array(counts)


def centred(own_key, extent, deviation, bound, cuts=(), kind=jnp.bfloat16):
    factor_of = levels(own_key, extent, cuts, -0.22, 0.18) if cuts else 1.0
    entries = jax.random.normal(own_key, extent, jnp.float32) * deviation * factor_of
    return jnp.minimum(jnp.maximum(entries, -bound), bound).astype(kind)


def gaussian_with(key, dims, width, bound, shards, heavy, kind=jnp.bfloat16):
    entries = width * jax.random.normal(key, dims, jnp.float32)
    if shards:
        entries = entries * levels(key, dims, shards, -0.22, 0.18)
    return jnp.clip(spiked(entries, jax.random.fold_in(key, 3), *heavy), -bound, bound).astype(kind)


def setup_inputs(seed: int = 0) -> dict:
    key_list = jax.random.split(jax.random.key(seed), 16)
    queries = draw_queries(jax.random.fold_in(key_list[15], 71), 0)
    keys = draw_keys(jax.random.fold_in(key_list[15], 71), 0)
    values = centred(key_list[2], (SEQ, QW), 1.0, 6.0, ((0, 8), (1, 4)))
    cum_gate = draw_cum_gate(jax.random.fold_in(key_list[15], 71), 0)
    head_gain = jnp.clip(1.0 + 0.18 * jax.random.normal(key_list[4], (QW,), jnp.float32), 0.1, 1.9)
    moe_in = centred(key_list[5], (MTOK, D), 1.0, 6.0, ((0, 8),))
    ffn_gain = jnp.clip(1.0 + 0.18 * jax.random.normal(key_list[6], (D,), jnp.float32), 0.1, 1.9)
    routes_keys = jax.random.split(jax.random.fold_in(key_list[7], 1), MTOK // MROWS)
    routes_turns = jax.random.permutation(jax.random.fold_in(key_list[7], 3), MTOK // MROWS)
    routes = jax.vmap(lambda own, number: assign_block(jax.random.fold_in(key_list[7], 2), own, number, MROWS, EXPERTS, TOP, CAP, 2))(routes_keys, routes_turns).reshape((MTOK, TOP))
    route_weight = jnp.clip(0.2 + 1 * jax.random.uniform(key_list[8], (MTOK, TOP), jnp.float32) ** levels(key_list[8], (MTOK, TOP), ((0, 8),), -0.2, 0.2), 0.2, 1.2)
    expert_gate = centred(key_list[9], (EXPERTS, FF_E, D), D ** -0.5, 0.125, ((0, 8), (1, 4)))
    expert_up = centred(key_list[10], (EXPERTS, FF_E, D), D ** -0.5, 0.125, ((0, 8), (1, 4)))
    expert_down = gaussian_with(key_list[11], (EXPERTS, FF_E, D), FF_E ** -0.5, 0.25, ((0, 8), (1, 4)), (1, 2, 4, 2.0))
    shared_gate = centred(key_list[12], (SHARED, D), D ** -0.5, 0.125, ((0, 4),))
    shared_up = centred(key_list[13], (SHARED, D), D ** -0.5, 0.125, ((0, 4),))
    shared_down = gaussian_with(key_list[14], (SHARED, D), SHARED ** -0.5, 0.375, ((0, 4),), (0, 1, 4, 2.0))
    return {"queries": queries, "keys": keys, "values": values, "cum_gate": cum_gate, "head_gain": head_gain, "moe_in": moe_in, "ffn_gain": ffn_gain, "routes": routes, "route_weight": route_weight, "expert_gate": expert_gate, "expert_up": expert_up, "expert_down": expert_down, "shared_gate": shared_gate, "shared_up": shared_up, "shared_down": shared_down}


NORM_EPSILON = 1e-06

def attend_head(head_inputs):
    query_head, key_head, value_head, gate_head = head_inputs
    block_len = math.gcd(SEQ, 512)
    positions = jnp.arange(SEQ, dtype=jnp.int32)
    score_scale = HEAD ** (-0.5)

    def one_block(block_num):
        first_row = block_num * block_len
        query_block = lax.dynamic_slice_in_dim(query_head, first_row, block_len, 0)
        gate_block = lax.dynamic_slice_in_dim(gate_head, first_row, block_len, 0)
        scores = jnp.dot(query_block, key_head.T, preferred_element_type=jnp.float32) * score_scale
        scores = scores + gate_block[:, None] - gate_head[None, :]
        query_pos = first_row + jnp.arange(block_len, dtype=jnp.int32)
        scores = jnp.where(positions[None, :] <= query_pos[:, None], scores, -jnp.inf)
        top_score = lax.optimization_barrier(jnp.max(scores, axis=1, keepdims=True))
        weights = jnp.exp(scores - top_score).astype(jnp.bfloat16)
        return jnp.dot(weights, value_head, preferred_element_type=jnp.float32)
    blocks = lax.map(one_block, jnp.arange(SEQ // block_len, dtype=jnp.int32))
    return blocks.reshape(SEQ, HEAD)

def blocked_down(hidden, weight):
    block_width = hidden.shape[1] // N_TP

    def add_block(running, block_num):
        start_col = block_num * block_width
        product = jnp.dot(lax.dynamic_slice_in_dim(hidden, start_col, block_width, 1), lax.dynamic_slice_in_dim(weight, start_col, block_width, 0), preferred_element_type=jnp.float32)
        rounded = lax.optimization_barrier(product.astype(jnp.bfloat16))
        return (running + rounded.astype(jnp.float32), None)
    start_sum = jnp.zeros((hidden.shape[0], weight.shape[1]), jnp.float32)
    result, _ = lax.scan(add_block, start_sum, jnp.arange(N_TP, dtype=jnp.int32))
    return result

def slot_index(route_rows):
    flat_routes = route_rows.reshape(-1)
    agreement_tally = (flat_routes[:, None] == jnp.arange(EXPERTS, dtype=jnp.int32)[None, :]).astype(jnp.int32)
    earlier = lax.optimization_barrier(jnp.sum((jnp.cumsum(agreement_tally, axis=0) - 1) * agreement_tally, axis=1))
    return (flat_routes * CAP + earlier).astype(jnp.int32)

def fill_slots(token_rows, slot_ids):
    owner_row = jnp.full((EXPERTS * CAP,), MROWS, jnp.int32).at[slot_ids].set(jnp.arange(MROWS * TOP, dtype=jnp.int32) // TOP)
    padded = jnp.concatenate([token_rows, jnp.zeros((1, D), token_rows.dtype)], axis=0)
    return padded[owner_row]

def run_expert(expert_inputs):
    rows_in, gate_weight, up_weight, down_weight = expert_inputs
    hidden = (jax.nn.silu(jnp.dot(rows_in, gate_weight.T, preferred_element_type=jnp.float32)) * jnp.dot(rows_in, up_weight.T, preferred_element_type=jnp.float32)).astype(jnp.bfloat16)
    return blocked_down(hidden, down_weight).astype(jnp.bfloat16)

def reference(queries, keys, values, cum_gate, head_gain, moe_in, ffn_gain, routes, route_weight, expert_gate, expert_up, expert_down, shared_gate, shared_up, shared_down):
    query_heads = queries.reshape(SEQ, HEADS, HEAD).transpose(1, 0, 2)
    key_heads = keys.reshape(SEQ, HEADS, HEAD).transpose(1, 0, 2)
    value_heads = values.reshape(SEQ, HEADS, HEAD).transpose(1, 0, 2)
    summed = lax.map(attend_head, (query_heads, key_heads, value_heads, cum_gate.T))
    mean_square = lax.optimization_barrier(jnp.mean(summed * summed, axis=2, keepdims=True))
    normed_heads = summed * lax.rsqrt(mean_square + NORM_EPSILON) * head_gain.reshape(HEADS, 1, HEAD)
    mixed = normed_heads.transpose(1, 0, 2).reshape(SEQ, QW).astype(jnp.bfloat16)
    source = moe_in.astype(jnp.float32)
    normed = (source * lax.rsqrt(lax.optimization_barrier(jnp.mean(source * source, axis=1, keepdims=True)) + NORM_EPSILON) * ffn_gain).astype(jnp.bfloat16)
    shared_hidden = (jax.nn.silu(jnp.dot(normed, shared_gate.T, preferred_element_type=jnp.float32)) * jnp.dot(normed, shared_up.T, preferred_element_type=jnp.float32)).astype(jnp.bfloat16)
    shared_sum = blocked_down(shared_hidden, shared_down)
    token_blocks = normed.reshape(N_EP, MROWS, D)
    route_blocks = routes.reshape(N_EP, MROWS, TOP)
    slot_ids = jax.vmap(slot_index)(route_blocks)
    buffers = jax.vmap(fill_slots)(token_blocks, slot_ids)
    by_expert = buffers.reshape(N_EP, EXPERTS, CAP, D).transpose(1, 0, 2, 3).reshape(EXPERTS, N_EP * CAP, D)
    results = lax.map(run_expert, (by_expert, expert_gate, expert_up, expert_down))
    returned = results.reshape(EXPERTS, N_EP, CAP, D).transpose(1, 0, 2, 3).reshape(N_EP, EXPERTS * CAP, D)
    picked = returned[jnp.arange(N_EP, dtype=jnp.int32)[:, None], slot_ids]
    picked = picked.reshape(MTOK, TOP, D).astype(jnp.float32)
    routed = lax.optimization_barrier(jnp.sum(picked * route_weight[:, :, None], axis=1))
    expert_out = (shared_sum + routed).astype(jnp.bfloat16)
    return (mixed, expert_out)
```

```python
import functools
import math

import jax
import jax.numpy as jnp
from jax import lax
from jax.experimental import pallas as pl
from jax.experimental.pallas import tpu as pltpu
from jax.sharding import PartitionSpec as P

NORM_EPSILON = 1e-06
VMEM = pltpu.VMEM


def swap_halves(x):
    half = x.shape[1] // 2
    return jnp.concatenate([x[:, half:], x[:, :half]], axis=1)


def pack_kernel(splits, scale, q_ref, k_ref, v_ref, kv_ref, qp_ref):
    rows, width = q_ref.shape
    tile = rows // splits
    half = tile // 2
    low = lax.broadcasted_iota(jnp.int32, (rows, 128), 1) < 64
    low_half = low[:half]
    for head in range(width // 64):
        lanes = slice(head // 2 * 128, head // 2 * 128 + 128)
        kc, vc = k_ref[:, lanes], v_ref[:, lanes]
        qc = q_ref[:, lanes] * jnp.asarray(scale, q_ref.dtype)
        if head % 2 == 0:
            kv_ref[head] = jnp.where(low, kc, swap_halves(vc))
        else:
            kv_ref[head] = jnp.where(low, swap_halves(kc), vc)
        for part in range(splits):
            a = qc[part * tile : part * tile + half]
            b = qc[part * tile + half : (part + 1) * tile]
            if head % 2 == 0:
                packed = jnp.where(low_half, a, swap_halves(b))
            else:
                packed = jnp.where(low_half, swap_halves(a), b)
            qp_ref[head * splits + part] = packed


def flash_kernel(splits, packed, key_len, q_ref, kv_ref, gate_ref, gain_ref, out_ref):
    block = pl.program_id(0)
    part = lax.rem(lax.axis_index("ep"), splits)
    raw = q_ref[0]
    half = raw.shape[0]
    if packed:
        low = lax.broadcasted_iota(jnp.int32, raw.shape, 1) < 64
        zero = jnp.zeros_like(raw)
        query = jnp.concatenate(
            [jnp.where(low, raw, zero), jnp.where(low, swap_halves(raw), zero)], axis=0
        )
    else:
        query = raw
    rows = query.shape[0]

    def visit(step, state, masked):
        peak, weighted = state
        keys = kv_ref[pl.ds(pl.multiple_of(step * key_len, key_len), key_len), :]
        scores = lax.dot_general(
            query, keys, (((1,), (1,)), ((), ())), preferred_element_type=jnp.float32
        )
        scores = scores - gate_ref[step]
        if masked:
            row_pos = part * rows + lax.broadcasted_iota(jnp.int32, scores.shape, 0)
            key_pos = lax.broadcasted_iota(jnp.int32, scores.shape, 1)
            scores = jnp.where(key_pos <= row_pos, scores, -jnp.inf)
        new_peak = jnp.maximum(peak, jnp.max(scores, axis=1, keepdims=True))
        weights = jnp.exp(scores - new_peak).astype(jnp.bfloat16)
        weighted = weighted * jnp.exp(peak - new_peak) + jnp.dot(
            weights, keys, preferred_element_type=jnp.float32
        )
        return new_peak, weighted

    state = (jnp.full((rows, 1), -1e30, jnp.float32), jnp.zeros((rows, 128), jnp.float32))
    state = visit(block, state, True)
    state = lax.fori_loop(0, block, lambda step, s: visit(step, s, False), state)
    _, weighted = state
    high = lax.broadcasted_iota(jnp.int32, weighted.shape, 1) >= 64
    square = jnp.sum(jnp.where(high, weighted * weighted, 0.0), axis=1, keepdims=True) / 64
    normed = weighted * lax.rsqrt(square + NORM_EPSILON) * gain_ref[...]
    if packed:
        normed = jnp.where(high[:half], normed[half:], swap_halves(normed[:half]))
    out_ref[0] = normed.astype(out_ref.dtype)


def attend(queries, keys, values, cum_gate, head_gain):
    rows, width = queries.shape
    heads = cum_gate.shape[1]
    size = width // heads
    devices = lax.axis_size("ep")
    splits = devices // heads
    tile = rows // splits
    scale = size**-0.5
    packed = heads % 2 == 0 and (tile // 2) % 16 == 0
    send_rows = tile // 2 if packed else tile
    if packed:
        kv, qp = pl.pallas_call(
            functools.partial(pack_kernel, splits, scale),
            out_shape=(
                jax.ShapeDtypeStruct((heads, rows, 128), jnp.bfloat16),
                jax.ShapeDtypeStruct((devices, send_rows, 128), jnp.bfloat16),
            ),
            name="pack",
        )(queries, keys, values)
    else:
        kv = jnp.concatenate(
            [keys.reshape(rows, heads, size), values.reshape(rows, heads, size)], axis=2
        ).transpose(1, 0, 2)
        qs = (queries * jnp.asarray(scale, queries.dtype)).reshape(splits, tile, heads, size)
        qs = qs.transpose(2, 0, 1, 3).reshape(devices, tile, size)
        qp = jnp.concatenate([qs, jnp.zeros_like(qs)], axis=2)
    parcel = jnp.concatenate([jnp.repeat(kv, splits, axis=0), qp], axis=1)
    gates = jnp.repeat(cum_gate.T, splits, axis=0)
    all_gates = lax.all_to_all(gates, "ep", split_axis=0, concat_axis=0, tiled=True)
    got = lax.all_to_all(parcel, "ep", split_axis=0, concat_axis=0, tiled=True)
    kv_all = got[:, :rows].reshape(devices * rows, 128)
    q_all = got[:, rows:]
    head = lax.axis_index("ep") // splits
    gain = lax.dynamic_slice_in_dim(head_gain, head * size, size, 0)
    gain = jnp.concatenate([gain, gain])[None]
    flops = 2 * 2 * 128 * devices * (devices + 1) // 2 * tile * rows
    out = pl.pallas_call(
        functools.partial(flash_kernel, splits, packed, rows),
        grid=(devices,),
        in_specs=[
            pl.BlockSpec((1, send_rows, 128), lambda i: (i, 0, 0)),
            pl.BlockSpec(memory_space=VMEM),
            pl.BlockSpec(memory_space=VMEM),
            pl.BlockSpec(memory_space=VMEM),
        ],
        out_specs=pl.BlockSpec((1, send_rows, 128), lambda i: (i, 0, 0)),
        out_shape=jax.ShapeDtypeStruct((devices, send_rows, 128), jnp.bfloat16),
        cost_estimate=pl.CostEstimate(
            flops=flops, bytes_accessed=4 * devices * rows * 128, transcendentals=flops // 512
        ),
        compiler_params=pltpu.CompilerParams(vmem_limit_bytes=40 << 20),
        name="flash",
    )(q_all, kv_all, all_gates.reshape(devices, 1, rows), gain)
    back = lax.all_to_all(out, "ep", split_axis=0, concat_axis=0, tiled=True)
    if packed:
        back = back.reshape(heads, splits, tile // 2, 2, size).transpose(1, 3, 2, 0, 4)
    else:
        back = back[:, :, size:].reshape(heads, splits, tile, size).transpose(1, 2, 0, 3)
    return back.reshape(rows, width)


def experts_half(
    moe_in,
    ffn_gain,
    routes,
    route_weight,
    expert_gate,
    expert_up,
    expert_down,
    shared_gate,
    shared_up,
    shared_down,
):
    tokens, model_width = moe_in.shape
    per_group, hidden_width = expert_gate.shape[:2]
    groups = lax.axis_size("ep")
    parts = lax.axis_size("tp")
    here = lax.axis_index("ep")
    slice_width = model_width // parts
    total = groups * tokens
    own_columns = lax.dynamic_slice_in_dim(
        moe_in, lax.axis_index("tp") * slice_width, slice_width, 1
    )
    gathered = lax.all_gather(own_columns, ("ep", "tp"), axis=0, tiled=True)
    source = (
        gathered.reshape(groups, parts, tokens, slice_width)
        .transpose(0, 2, 1, 3)
        .reshape(total, model_width)
        .astype(jnp.float32)
    )
    normed = (
        source
        * lax.rsqrt(jnp.mean(source * source, axis=1, keepdims=True) + NORM_EPSILON)
        * ffn_gain
    ).astype(jnp.bfloat16)
    all_routes = lax.all_gather(routes, "ep", axis=0, tiled=True)
    all_weights = lax.all_gather(route_weight, "ep", axis=0, tiled=True)
    mine = here * per_group + jnp.arange(per_group, dtype=jnp.int32)
    share = jnp.sum(
        jnp.where(all_routes[:, :, None] == mine, all_weights[:, :, None], 0.0), axis=1
    )

    def product(left, right):
        return lax.dot_general(
            left, right, (((1,), (1,)), ((), ())), preferred_element_type=jnp.float32
        )

    gate_value = product(normed, expert_gate.reshape(-1, model_width))
    up_value = product(normed, expert_up.reshape(-1, model_width))
    hidden = jax.nn.silu(gate_value) * up_value
    hidden = hidden.reshape(total, per_group, hidden_width) * share[:, :, None]
    hidden = hidden.reshape(total, -1).astype(jnp.bfloat16)
    own = lax.dynamic_slice_in_dim(normed, here * tokens, tokens, 0)
    shared_hidden = (jax.nn.silu(product(own, shared_gate)) * product(own, shared_up)).astype(
        jnp.bfloat16
    )
    shared_term = jnp.dot(shared_hidden, shared_down, preferred_element_type=jnp.float32)
    term = jnp.dot(
        hidden, expert_down.reshape(-1, model_width), preferred_element_type=jnp.float32
    ).reshape(groups, tokens, model_width)
    is_own = (jnp.arange(groups, dtype=jnp.int32) == here)[:, None, None]
    term = (term + jnp.where(is_own, shared_term[None], 0.0)).astype(jnp.bfloat16)
    blocks = (
        term.reshape(groups, tokens, parts, slice_width)
        .transpose(0, 2, 1, 3)
        .reshape(groups * parts * tokens, slice_width)
    )
    return lax.psum_scatter(blocks, ("ep", "tp"), scatter_dimension=0, tiled=True)


def on_device(
    queries,
    keys,
    values,
    cum_gate,
    head_gain,
    moe_in,
    ffn_gain,
    routes,
    route_weight,
    expert_gate,
    expert_up,
    expert_down,
    shared_gate,
    shared_up,
    shared_down,
):
    expert_out = experts_half(
        moe_in,
        ffn_gain,
        routes,
        route_weight,
        expert_gate,
        expert_up,
        expert_down,
        shared_gate,
        shared_up,
        shared_down,
    )
    mixed = attend(queries, keys, values, cum_gate, head_gain)
    return (mixed, expert_out)


def solution(mesh):
    in_specs = (
        P("ep", "tp"),
        P("ep", "tp"),
        P("ep", "tp"),
        P("ep", "tp"),
        P("tp"),
        P("ep", None),
        P(),
        P("ep", None),
        P("ep", None),
        P("ep", "tp", None),
        P("ep", "tp", None),
        P("ep", "tp", None),
        P("tp", None),
        P("tp", None),
        P("tp", None),
    )
    out_specs = (P("ep", "tp"), P("ep", "tp"))
    return jax.shard_map(
        on_device, mesh=mesh, in_specs=in_specs, out_specs=out_specs, check_vma=False
    )
```

```python
import functools
import math

import jax
import jax.numpy as jnp
from jax import lax
from jax.experimental import pallas as pl
from jax.experimental.pallas import tpu as pltpu
from jax.sharding import PartitionSpec as P

NORM_EPSILON = 1e-06
VMEM = pltpu.VMEM


def swap_halves(x):
    half = x.shape[1] // 2
    return jnp.concatenate([x[:, half:], x[:, :half]], axis=1)


def pack_kernel(splits, scale, q_ref, k_ref, v_ref, kv_ref, qp_ref):
    rows, width = q_ref.shape
    tile = rows // splits
    half = tile // 2
    low = lax.broadcasted_iota(jnp.int32, (rows, 128), 1) < 64
    low_half = low[:half]
    for head in range(width // 64):
        lanes = slice(head // 2 * 128, head // 2 * 128 + 128)
        kc, vc = k_ref[:, lanes], v_ref[:, lanes]
        qc = q_ref[:, lanes] * jnp.asarray(scale, q_ref.dtype)
        if head % 2 == 0:
            kv_ref[head] = jnp.where(low, kc, swap_halves(vc))
        else:
            kv_ref[head] = jnp.where(low, swap_halves(kc), vc)
        for part in range(splits):
            a = qc[part * tile : part * tile + half]
            b = qc[part * tile + half : (part + 1) * tile]
            if head % 2 == 0:
                packed = jnp.where(low_half, a, swap_halves(b))
            else:
                packed = jnp.where(low_half, swap_halves(a), b)
            qp_ref[head * splits + part] = packed


def flash_kernel(splits, packed, key_len, q_ref, kv_ref, gate_ref, gain_ref, out_ref):
    block = pl.program_id(0)
    part = lax.rem(lax.axis_index("ep"), splits)
    raw = q_ref[0]
    half = raw.shape[0]
    if packed:
        low = lax.broadcasted_iota(jnp.int32, raw.shape, 1) < 64
        zero = jnp.zeros_like(raw)
        query = jnp.concatenate(
            [jnp.where(low, raw, zero), jnp.where(low, swap_halves(raw), zero)], axis=0
        )
    else:
        query = raw
    rows = query.shape[0]

    def visit(step, state, masked):
        peak, weighted = state
        keys = kv_ref[pl.ds(pl.multiple_of(step * key_len, key_len), key_len), :]
        scores = lax.dot_general(
            query, keys, (((1,), (1,)), ((), ())), preferred_element_type=jnp.float32
        )
        scores = scores - gate_ref[step]
        if masked:
            row_pos = part * rows + lax.broadcasted_iota(jnp.int32, scores.shape, 0)
            key_pos = lax.broadcasted_iota(jnp.int32, scores.shape, 1)
            scores = jnp.where(key_pos <= row_pos, scores, -jnp.inf)
        new_peak = jnp.maximum(peak, jnp.max(scores, axis=1, keepdims=True))
        weights = jnp.exp(scores - new_peak).astype(jnp.bfloat16)
        weighted = weighted * jnp.exp(peak - new_peak) + jnp.dot(
            weights, keys, preferred_element_type=jnp.float32
        )
        return new_peak, weighted

    state = (jnp.full((rows, 1), -1e30, jnp.float32), jnp.zeros((rows, 128), jnp.float32))
    state = visit(block, state, True)
    state = lax.fori_loop(0, block, lambda step, s: visit(step, s, False), state)
    _, weighted = state
    high = lax.broadcasted_iota(jnp.int32, weighted.shape, 1) >= 64
    square = jnp.sum(jnp.where(high, weighted * weighted, 0.0), axis=1, keepdims=True) / 64
    normed = weighted * lax.rsqrt(square + NORM_EPSILON) * gain_ref[...]
    if packed:
        normed = jnp.where(high[:half], normed[half:], swap_halves(normed[:half]))
    out_ref[0] = normed.astype(out_ref.dtype)


def trade_small(cum_gate, routes, route_weight):
    rows, heads = cum_gate.shape
    devices = lax.axis_size("ep")
    tokens, choose = routes.shape
    gates = jnp.repeat(cum_gate.T, devices // heads, axis=0)
    named = jnp.concatenate([routes.astype(jnp.float32).reshape(-1), route_weight.reshape(-1)])
    small = jnp.concatenate([gates, jnp.broadcast_to(named, (devices, named.size))], axis=1)
    small = lax.all_to_all(small, "ep", split_axis=0, concat_axis=0, tiled=True)
    count = tokens * choose
    all_routes = small[:, rows : rows + count].astype(jnp.int32).reshape(-1, choose)
    all_weights = small[:, rows + count :].reshape(-1, choose)
    return small[:, :rows], all_routes, all_weights


def trade_rows(queries, keys, values, heads):
    rows, width = queries.shape
    size = width // heads
    devices = lax.axis_size("ep")
    splits = devices // heads
    tile = rows // splits
    scale = size**-0.5
    packed = heads % 2 == 0 and (tile // 2) % 16 == 0
    send_rows = tile // 2 if packed else tile
    if packed:
        kv, qp = pl.pallas_call(
            functools.partial(pack_kernel, splits, scale),
            out_shape=(
                jax.ShapeDtypeStruct((heads, rows, 128), jnp.bfloat16),
                jax.ShapeDtypeStruct((devices, send_rows, 128), jnp.bfloat16),
            ),
            name="pack",
        )(queries, keys, values)
    else:
        kv = jnp.concatenate(
            [keys.reshape(rows, heads, size), values.reshape(rows, heads, size)], axis=2
        ).transpose(1, 0, 2)
        qs = (queries * jnp.asarray(scale, queries.dtype)).reshape(splits, tile, heads, size)
        qs = qs.transpose(2, 0, 1, 3).reshape(devices, tile, size)
        qp = jnp.concatenate([qs, jnp.zeros_like(qs)], axis=2)
    parcel = jnp.concatenate([jnp.repeat(kv, splits, axis=0), qp], axis=1)
    return lax.all_to_all(parcel, "ep", split_axis=0, concat_axis=0, tiled=True), packed


def attend(got, packed, rows, all_gates, heads, head_gain):
    devices, parcel_rows, _ = got.shape
    width = head_gain.shape[0]
    size = width // heads
    splits = devices // heads
    tile = rows // splits
    send_rows = parcel_rows - rows
    kv_all = got[:, :rows].reshape(devices * rows, 128)
    q_all = got[:, rows:]
    head = lax.axis_index("ep") // splits
    gain = lax.dynamic_slice_in_dim(head_gain, head * size, size, 0)
    gain = jnp.concatenate([gain, gain])[None]
    flops = 2 * 2 * 128 * devices * (devices + 1) // 2 * tile * rows
    out = pl.pallas_call(
        functools.partial(flash_kernel, splits, packed, rows),
        grid=(devices,),
        in_specs=[
            pl.BlockSpec((1, send_rows, 128), lambda i: (i, 0, 0)),
            pl.BlockSpec(memory_space=VMEM),
            pl.BlockSpec(memory_space=VMEM),
            pl.BlockSpec(memory_space=VMEM),
        ],
        out_specs=pl.BlockSpec((1, send_rows, 128), lambda i: (i, 0, 0)),
        out_shape=jax.ShapeDtypeStruct((devices, send_rows, 128), jnp.bfloat16),
        cost_estimate=pl.CostEstimate(
            flops=flops, bytes_accessed=4 * devices * rows * 128, transcendentals=flops // 512
        ),
        compiler_params=pltpu.CompilerParams(vmem_limit_bytes=40 << 20),
        name="flash",
    )(q_all, kv_all, all_gates.reshape(devices, 1, rows), gain)
    back = lax.all_to_all(out, "ep", split_axis=0, concat_axis=0, tiled=True)
    if packed:
        back = back.reshape(heads, splits, tile // 2, 2, size).transpose(1, 3, 2, 0, 4)
    else:
        back = back[:, :, size:].reshape(heads, splits, tile, size).transpose(1, 2, 0, 3)
    return back.reshape(rows, width)


def norm_kernel(x_ref, gain_ref, out_ref):
    parts, _, width = x_ref.shape
    pieces = [x_ref[part].astype(jnp.float32) for part in range(parts)]
    square = sum(jnp.sum(p * p, axis=1, keepdims=True) for p in pieces) / (parts * width)
    factor = lax.rsqrt(square + NORM_EPSILON)
    for part, piece in enumerate(pieces):
        lanes = slice(part * width, (part + 1) * width)
        out_ref[:, lanes] = (piece * factor * gain_ref[:, lanes]).astype(out_ref.dtype)


def gated(rows, gate, up):
    dims = (((1,), (1,)), ((), ()))
    gate_value = lax.dot_general(rows, gate, dims, preferred_element_type=jnp.float32)
    up_value = lax.dot_general(rows, up, dims, preferred_element_type=jnp.float32)
    return gate_value / (1.0 + jnp.exp(-gate_value)) * up_value


def hidden_kernel(
    x_ref, routes_ref, weight_ref, gate_ref, up_ref, sgate_ref, sup_ref, hid_ref, shid_ref
):
    expert = pl.program_id(0)
    here = lax.axis_index("ep")
    tokens = shid_ref.shape[0]
    number = here * pl.num_programs(0) + expert
    chunk = min(256, x_ref.shape[0])

    @pl.loop(0, x_ref.shape[0] // chunk)
    def _(step):
        rows = pl.ds(pl.multiple_of(step * chunk, chunk), chunk)
        share = jnp.sum(
            jnp.where(routes_ref[rows, :] == number, weight_ref[rows, :], 0.0),
            axis=1,
            keepdims=True,
        )
        value = gated(x_ref[rows, :], gate_ref[0], up_ref[0])
        hid_ref[0, rows, :] = (value * share).astype(hid_ref.dtype)

    @pl.when(expert == 0)
    def _():
        own = x_ref[pl.ds(pl.multiple_of(here * tokens, tokens), tokens), :]
        shid_ref[...] = gated(own, sgate_ref[...], sup_ref[...]).astype(shid_ref.dtype)


def down_kernel(hid_ref, shid_ref, down_ref, sdown_ref, out_ref):
    tokens = shid_ref.shape[0]
    here = lax.axis_index("ep")
    per_group = down_ref.shape[0]

    @pl.loop(0, hid_ref.shape[1] // tokens)
    def _(step):
        rows = pl.ds(pl.multiple_of(step * tokens, tokens), tokens)
        term = sum(
            jnp.dot(hid_ref[expert, rows, :], down_ref[expert], preferred_element_type=jnp.float32)
            for expert in range(per_group)
        )
        out_ref[0, rows, :] = term.astype(out_ref.dtype)

        @pl.when(step == here)
        def _():
            extra = jnp.dot(shid_ref[...], sdown_ref[...], preferred_element_type=jnp.float32)
            out_ref[0, rows, :] = (term + extra).astype(out_ref.dtype)


def gather_tokens(moe_in):
    slice_width = moe_in.shape[1] // lax.axis_size("tp")
    own_columns = lax.dynamic_slice_in_dim(
        moe_in, lax.axis_index("tp") * slice_width, slice_width, 1
    )
    return lax.all_gather(own_columns, ("ep", "tp"), axis=0)


def expert_terms(
    gathered,
    ffn_gain,
    all_routes,
    all_weights,
    expert_gate,
    expert_up,
    expert_down,
    shared_gate,
    shared_up,
    shared_down,
):
    tokens = gathered.shape[1]
    model_width = ffn_gain.shape[0]
    per_group, hidden_width = expert_gate.shape[:2]
    shared_width = shared_gate.shape[0]
    groups = lax.axis_size("ep")
    parts = lax.axis_size("tp")
    slice_width = model_width // parts
    total = groups * tokens
    params = pltpu.CompilerParams(vmem_limit_bytes=48 << 20)
    whole = pl.BlockSpec(memory_space=VMEM)
    normed = pl.pallas_call(
        norm_kernel,
        grid=(groups,),
        in_specs=[pl.BlockSpec((parts, tokens, slice_width), lambda i: (i, 0, 0)), whole],
        out_specs=pl.BlockSpec((tokens, model_width), lambda i: (i, 0)),
        out_shape=jax.ShapeDtypeStruct((total, model_width), jnp.bfloat16),
        cost_estimate=pl.CostEstimate(
            flops=4 * total * model_width, bytes_accessed=4 * total * model_width, transcendentals=0
        ),
        name="norm",
    )(gathered, ffn_gain[None])
    weight_spec = pl.BlockSpec((1, hidden_width, model_width), lambda i: (i, 0, 0))
    columns = per_group * hidden_width
    hidden, shared_hidden = pl.pallas_call(
        hidden_kernel,
        grid=(per_group,),
        in_specs=[whole, whole, whole, weight_spec, weight_spec, whole, whole],
        out_specs=(
            pl.BlockSpec((1, total, hidden_width), lambda i: (i, 0, 0)),
            pl.BlockSpec((tokens, shared_width), lambda i: (0, 0)),
        ),
        out_shape=(
            jax.ShapeDtypeStruct((per_group, total, hidden_width), jnp.bfloat16),
            jax.ShapeDtypeStruct((tokens, shared_width), jnp.bfloat16),
        ),
        cost_estimate=pl.CostEstimate(
            flops=4 * total * model_width * columns,
            bytes_accessed=4 * columns * model_width,
            transcendentals=total * columns,
        ),
        compiler_params=params,
        name="hidden",
    )(normed, all_routes, all_weights, expert_gate, expert_up, shared_gate, shared_up)
    return pl.pallas_call(
        down_kernel,
        grid=(parts,),
        in_specs=[
            whole,
            whole,
            pl.BlockSpec((per_group, hidden_width, slice_width), lambda i: (0, 0, i)),
            pl.BlockSpec((shared_width, slice_width), lambda i: (0, i)),
        ],
        out_specs=pl.BlockSpec((1, total, slice_width), lambda i: (i, 0, 0)),
        out_shape=jax.ShapeDtypeStruct((parts, total, slice_width), jnp.bfloat16),
        cost_estimate=pl.CostEstimate(
            flops=2 * total * model_width * columns,
            bytes_accessed=2 * (columns + total) * model_width,
            transcendentals=0,
        ),
        compiler_params=params,
        name="down",
    )(hidden, shared_hidden, expert_down, shared_down)


def combine_terms(term):
    groups = lax.axis_size("ep")
    _, total, slice_width = term.shape
    tokens = total // groups
    summed = lax.psum_scatter(term, "tp", scatter_dimension=0, tiled=True)
    back = lax.all_to_all(
        summed.reshape(groups, tokens, slice_width), "ep", split_axis=0, concat_axis=0, tiled=True
    )
    return jnp.sum(back.astype(jnp.float32), axis=0).astype(jnp.bfloat16)


def on_device(
    queries,
    keys,
    values,
    cum_gate,
    head_gain,
    moe_in,
    ffn_gain,
    routes,
    route_weight,
    expert_gate,
    expert_up,
    expert_down,
    shared_gate,
    shared_up,
    shared_down,
):
    rows, heads = cum_gate.shape
    gathered = gather_tokens(moe_in)
    got, packed = trade_rows(queries, keys, values, heads)
    all_gates, all_routes, all_weights = trade_small(cum_gate, routes, route_weight)
    gathered, got = lax.optimization_barrier((gathered, got))
    term = expert_terms(
        gathered,
        ffn_gain,
        all_routes,
        all_weights,
        expert_gate,
        expert_up,
        expert_down,
        shared_gate,
        shared_up,
        shared_down,
    )
    term, got = lax.optimization_barrier((term, got))
    mixed = attend(got, packed, rows, all_gates, heads, head_gain)
    return (mixed, combine_terms(term))


def solution(mesh):
    in_specs = (
        P("ep", "tp"),
        P("ep", "tp"),
        P("ep", "tp"),
        P("ep", "tp"),
        P("tp"),
        P("ep", None),
        P(),
        P("ep", None),
        P("ep", None),
        P("ep", "tp", None),
        P("ep", "tp", None),
        P("ep", "tp", None),
        P("tp", None),
        P("tp", None),
        P("tp", None),
    )
    out_specs = (P("ep", "tp"), P("ep", "tp"))
    return jax.shard_map(
        on_device, mesh=mesh, in_specs=in_specs, out_specs=out_specs, check_vma=False
    )
```
